32 devices in a mesh: kv: 4 (over y, x), tp: 8 (over z, core).
Axes of the slice: x: 2, y: 2, z: 4, core: 2. Of those that a mesh axis runs over, the one named last changes fastest.
Arguments:
- hidden_in: bfloat16 [16, 4096], P('kv', 'tp'), may hold values from -12 to 12
- mixer_gain: float32 [4096], P('tp'), may hold values from 0.1 to 1.9
- query_weight: bfloat16 [4096, 4096], P('tp', 'kv'), may hold values from -0.09375 to 0.09375
- key_weight: bfloat16 [4096, 4096], P('tp', 'kv'), may hold values from -0.09375 to 0.09375
- value_weight: bfloat16 [4096, 8192], P('tp', 'kv'), may hold values from -0.09375 to 0.09375
- gate_weight: bfloat16 [4096, 8192], P('tp', 'kv'), may hold values from -0.09375 to 0.09375
- decay_rate: float32 [16], P('kv'), may hold values from 0.0005 to 0.15
- prior_state: float32 [16, 16, 256, 512], P('tp', 'kv'), may hold values from -2.5 to 2.5
- key_block: bfloat16 [16, 16, 128, 256], P('tp', 'kv'), may hold values from -1 to 1
- value_block: bfloat16 [16, 16, 128, 512], P('tp', 'kv'), may hold values from -6 to 6
- lengths: int32 [16], P('tp'), may hold values from 1 to 16384, 65536 in all
- group_gain: float32 [8192], P('kv'), may hold values from 0.1 to 1.9
- output_weight: bfloat16 [8192, 4096], P('kv', 'tp'), may hold values from -0.0625 to 0.0625
- channel_gain: float32 [4096], P('tp'), may hold values from 0.1 to 1.9
- hidden_gate: bfloat16 [4096, 11264], P('tp', 'kv'), may hold values from -0.09375 to 0.09375
- hidden_up: bfloat16 [4096, 11264], P('tp', 'kv'), may hold values from -0.09375 to 0.09375
- hidden_down: bfloat16 [11264, 4096], P('kv', 'tp'), may hold values from -0.0546875 to 0.0546875
Outputs:
- layer_out: bfloat16 [16, 4096], P('kv', 'tp')
The draws below stay inside these ranges and needn't reach their ends.
Inputs may be any that keep to these rules, and one draw needn't show every extreme that they name: Sequence s has lengths[s] earlier positions; slots 0 to (lengths[s] mod 128) - 1 of key_block and value_block hold the turned, scaled keys and the values of its positions from 128 * floor(lengths[s] / 128) on, prior_state holds the state of the positions before them, and the other slots take no part.
All inputs are finite; a program needn't handle non-finite values. No bound on the sum of `lengths` on one device may be relied on, other than what follows from the above.
Results may differ from the reference program's by a relative error of at most 0.029.
Values may be sent and summed in bfloat16 or wider, within the bound.
A program may use at most 64 MiB of HBM per device.

```python
import math
import jax
import jax.numpy as jnp
import numpy as np
from jax import lax

D = 4096
HEADS = 16
DK = 256
DV = 512
FF = 11264
BLK = 128
MEAN_LEN = 4096
MOST_LEN = 16384
SEQS = 16


def draw_hidden_in(key, part):
    columns = jnp.arange(D, dtype=jnp.float32) / D
    column_scale = 0.4 * jnp.exp(jnp.log(5.0) * columns)
    base_key = jax.random.fold_in(key, 11)
    base = jnp.clip(jax.random.normal(base_key, (SEQS, D), jnp.float32), -6.0, 6.0)
    return (base * column_scale[None, :]).astype(jnp.bfloat16)


def draw_decay_rate(key, part):
    lowest_rate = 0.003
    highest_rate = 0.15
    uniform_unit = jax.random.uniform(jax.random.fold_in(key, 21), (HEADS,), jnp.float32)
    return jnp.exp(jnp.log(lowest_rate) + uniform_unit * (jnp.log(highest_rate) - jnp.log(lowest_rate)))


def steps_of(own_key, extent, pieces, smallest, high):
    gain = 1.0
    for dim, shards_of in pieces:
        draws = jax.random.uniform(jax.random.fold_in(jax.random.fold_in(own_key, 6), dim), (shards_of,), jnp.float32, smallest / len(pieces), high / len(pieces))
        gain = gain * jnp.repeat(jnp.exp(draws), extent[dim] // shards_of).reshape((-1,) + (1,) * (len(extent) - 1 - dim))
    return gain


def length_profile(number_of, total, limit, lean):
    weights = [(1 << 20) // math.isqrt(standing ** lean) + 1 for standing in range(2, number_of + 1)]
    spare, counts = total - limit - (number_of - 1), [1] * (number_of - 1)
    while spare > 0:
        free = [i for i in range(number_of - 1) if counts[i] < limit]
        whole, budget = sum([weights[i] for i in free]), spare
        for i in free:
            extra = min(limit - counts[i], max(1, budget * weights[i] // whole), spare)
            counts[i] = counts[i] + extra
            spare = spare - extra
    return np.array([limit] + counts)


def uneven_parts(key, number_of, total, limit, skew):
    if number_of == 2:
        one = jax.random.randint(key, (), max(1, total - limit), min(limit, total - 1) + 1)
        return jnp.stack([one, total - one])
    sizes = jnp.asarray(length_profile(number_of, total, limit, skew), jnp.int32)
    couples = (number_of - 1) // 2
    giver, taker = sizes[1:1 + 2 * couples:2], sizes[2:2 + 2 * couples:2]
    room = jnp.minimum(giver - 1, limit - taker)
    shifted = jax.random.randint(jax.random.fold_in(key, 1), (couples,), 0, 1 << 20) % (room + 1)
    sizes = sizes.at[1:1 + 2 * couples:2].set(giver - shifted).at[2:2 + 2 * couples:2].set(taker + shifted)
    return sizes[jax.random.permutation(jax.random.fold_in(key, 2), number_of)]


def bell_draw(stream_key, extent, deviation, limit, split=(), kind=jnp.bfloat16):
    drawn = jax.random.normal(stream_key, extent, jnp.float32) * deviation
    if len(split) > 0:
        drawn = steps_of(stream_key, extent, split, -0.22, 0.18) * drawn
    return jnp.clip(drawn, min=-limit, max=limit).astype(kind)


def setup_inputs(seed: int = 0) -> dict:
    keys = jax.random.split(jax.random.key(seed), 18)
    return {
        "hidden_in": draw_hidden_in(jax.random.fold_in(keys[17], 71), 0),
        "mixer_gain": jnp.clip(1.0 + 0.18 * jax.random.normal(keys[1], (D,), jnp.float32), 0.1, 1.9),
        "query_weight": bell_draw(keys[2], (D, HEADS * DK), D ** -0.5, 0.09375, ((0, 8), (1, 4))),
        "key_weight": bell_draw(keys[3], (D, HEADS * DK), D ** -0.5, 0.09375, ((0, 8), (1, 4))),
        "value_weight": bell_draw(keys[4], (D, HEADS * DV), D ** -0.5, 0.09375, ((0, 8), (1, 4))),
        "gate_weight": bell_draw(keys[5], (D, HEADS * DV), D ** -0.5, 0.09375, ((0, 8), (1, 4))),
        "decay_rate": draw_decay_rate(jax.random.fold_in(keys[17], 71), 0),
        "prior_state": bell_draw(keys[7], (SEQS, HEADS, DK, DV), 0.3, 2.5, ((0, 8), (1, 4)), jnp.float32),
        "key_block": bell_draw(keys[8], (SEQS, HEADS, BLK, DK), 0.0625, 1.0, ((0, 8), (1, 4))),
        "value_block": bell_draw(keys[9], (SEQS, HEADS, BLK, DV), 1.0, 6.0, ((0, 8), (1, 4))),
        "lengths": uneven_parts(keys[10], SEQS, SEQS * MEAN_LEN, MOST_LEN, 2).astype(jnp.int32),
        "group_gain": jnp.clip(1.0 + 0.18 * jax.random.normal(keys[11], (HEADS * DV,), jnp.float32), 0.1, 1.9),
        "output_weight": bell_draw(keys[12], (HEADS * DV, D), (HEADS * DV) ** -0.5, 0.0625, ((0, 4), (1, 8))),
        "channel_gain": jnp.clip(1.0 + 0.18 * jax.random.normal(keys[13], (D,), jnp.float32), 0.1, 1.9),
        "hidden_gate": bell_draw(keys[14], (D, FF), D ** -0.5, 0.09375, ((0, 8), (1, 4))),
        "hidden_up": bell_draw(keys[15], (D, FF), D ** -0.5, 0.09375, ((0, 8), (1, 4))),
        "hidden_down": bell_draw(keys[16], (FF, D), FF ** -0.5, 0.0546875, ((0, 4), (1, 8))),
    }


epsilon = 1e-06

def rotate(vectors, position):
    half_dim = vectors.shape[-1] // 2
    inverse = 10000.0 ** (-jnp.arange(half_dim, dtype=jnp.float32) / half_dim)
    angles = position.astype(jnp.float32)[:, None, None] * inverse
    cosine_part = jnp.cos(angles)
    sine_part = jnp.sin(angles)
    front_half = vectors[..., :half_dim]
    back_half = vectors[..., half_dim:]
    return jnp.concatenate([front_half * cosine_part - back_half * sine_part, front_half * sine_part + back_half * cosine_part], axis=-1)

def retain(queries, keys_new, values_new, gates, decay_rate, prior_state, key_block, value_block, lengths, group_gain):
    batch_rows = queries.shape[0]
    heads_here = decay_rate.shape[0]
    key_width = prior_state.shape[2]
    value_width = prior_state.shape[3]
    block_len = key_block.shape[2]
    rotated = rotate(queries.astype(jnp.float32).reshape(batch_rows, heads_here, key_width), lengths).astype(jnp.bfloat16)
    fresh_keys = rotate(keys_new.astype(jnp.float32).reshape(batch_rows, heads_here, key_width), lengths) * key_width ** (-0.5)
    fresh_values = values_new.astype(jnp.float32).reshape(batch_rows, heads_here, value_width)
    filled = (lengths % block_len).astype(jnp.int32)
    slots = jnp.arange(block_len, dtype=jnp.int32)
    distance = (filled[:, None] - slots[None, :]).astype(jnp.float32)
    live_slots = (slots[None, :] < filled[:, None])[:, None, :]
    weighting = jnp.where(live_slots, jnp.exp(-decay_rate[None, :, None] * distance[:, None, :]), jnp.float32(0.0))
    rotated_wide = rotated.astype(jnp.float32)
    scores = jnp.einsum('shk,shjk->shj', rotated_wide, key_block.astype(jnp.float32))
    block_weights = (scores * weighting).astype(jnp.bfloat16)
    block_term = jnp.einsum('shj,shjv->shv', block_weights.astype(jnp.float32), value_block.astype(jnp.float32))
    own_term = lax.optimization_barrier(jnp.sum(rotated_wide * fresh_keys, axis=-1, keepdims=True)) * fresh_values
    carried = jnp.exp(-decay_rate[None, :, None] * (filled[:, None, None] + 1).astype(jnp.float32))
    state_term = carried * jnp.einsum('shk,shkv->shv', rotated_wide, prior_state, precision=lax.Precision.HIGHEST)
    retained = own_term + block_term + state_term
    centre = lax.optimization_barrier(jnp.mean(retained, axis=-1, keepdims=True))
    spread = lax.optimization_barrier(jnp.mean(jnp.square(retained - centre), axis=-1, keepdims=True))
    normed = (retained - centre) * lax.rsqrt(spread + epsilon)
    gated = jax.nn.silu(gates.astype(jnp.float32)).reshape(batch_rows, heads_here, value_width) * normed * group_gain.reshape(heads_here, value_width)
    return gated.astype(jnp.bfloat16).reshape(batch_rows, heads_here * value_width)

def reference(hidden_in, mixer_gain, query_weight, key_weight, value_weight, gate_weight, decay_rate, prior_state, key_block, value_block, lengths, group_gain, output_weight, channel_gain, hidden_gate, hidden_up, hidden_down):
    stream = hidden_in.astype(jnp.float32)
    first_scale = lax.rsqrt(lax.optimization_barrier(jnp.mean(stream * stream, axis=1, keepdims=True)) + epsilon)
    scaled_in = (stream * mixer_gain).astype(jnp.bfloat16)
    queries = (first_scale * jnp.dot(scaled_in, query_weight, preferred_element_type=jnp.float32)).astype(jnp.bfloat16)
    keys_new = (first_scale * jnp.dot(scaled_in, key_weight, preferred_element_type=jnp.float32)).astype(jnp.bfloat16)
    values_new = (first_scale * jnp.dot(scaled_in, value_weight, preferred_element_type=jnp.float32)).astype(jnp.bfloat16)
    gates = (first_scale * jnp.dot(scaled_in, gate_weight, preferred_element_type=jnp.float32)).astype(jnp.bfloat16)
    mixed = retain(queries, keys_new, values_new, gates, decay_rate, prior_state, key_block, value_block, lengths, group_gain)
    middle = stream + jnp.dot(mixed, output_weight, preferred_element_type=jnp.float32)
    second_scale = lax.rsqrt(lax.optimization_barrier(jnp.mean(middle * middle, axis=1, keepdims=True)) + epsilon)
    scaled_mid = (middle * channel_gain).astype(jnp.bfloat16)
    gate_part = second_scale * jnp.dot(scaled_mid, hidden_gate, preferred_element_type=jnp.float32)
    up_part = second_scale * jnp.dot(scaled_mid, hidden_up, preferred_element_type=jnp.float32)
    activated = (jax.nn.silu(gate_part) * up_part).astype(jnp.bfloat16)
    return (middle + jnp.dot(activated, hidden_down, preferred_element_type=jnp.float32)).astype(jnp.bfloat16)
```

```python
import functools

import jax
import jax.numpy as jnp
from jax import lax
from jax.experimental import pallas as pl
from jax.experimental.pallas import tpu as pltpu
from jax.sharding import PartitionSpec as P

EPS = 1e-06
MESH = pl.DeviceIdType.MESH
F32 = jnp.float32
BF16 = jnp.bfloat16


def up128(n):
    return (n + 127) // 128 * 128


def col_tiles(n, width=512):
    return [(c, min(width, n - c)) for c in range(0, n, width)]


def layer_kernel(
    n_kv, n_tp, H,
    hid, mg, wq, wk, wv, wg, decay, state, kblk, vblk, lens, gg, wo, cg, wgate, wup, wdown, cos, sin,
    out,
    hslots, vq, vk, vv, vg, st, kbv, vbv, vo, vgate, vup, vdown,
    x16, part, sA, rA, sB, rB, qs, ks, vs, gs, ts, mx, mx16, oS, oR, mid, sC, rC, ac, ac16, fS, fR,
    lsem, ssem, rsem,
):
    a = lax.axis_index("kv")
    b = lax.axis_index("tp")
    R, F = hid.shape
    S = lens.shape[0]
    rows = R * n_kv
    DK = state.shape[2]
    DV = state.shape[3]
    BLK = kblk.shape[2]
    FL = wgate.shape[1]
    FP = up128(FL)
    D = F * n_tp
    half = DK // 2

    loads = [
        pltpu.make_async_copy(src, dst, lsem.at[i])
        for i, (src, dst) in enumerate(
            [
                (hid, hslots.at[a]), (wq, vq), (wk, vk), (wv, vv), (wg, vg), (state, st),
                (kblk, kbv), (vblk, vbv), (wo, vo), (wgate, vgate), (wup, vup), (wdown, vdown),
            ]
        )
    ]
    for c in loads:
        c.start()

    barrier = pltpu.get_barrier_semaphore()
    for j in range(1, n_kv):
        pl.semaphore_signal(barrier, inc=1, device_id={"kv": lax.rem(a + j, n_kv)}, device_id_type=MESH)
    for j in range(1, n_tp):
        pl.semaphore_signal(barrier, inc=1, device_id={"tp": lax.rem(b + j, n_tp)}, device_id_type=MESH)
    pl.semaphore_wait(barrier, n_kv + n_tp - 2)

    def gather(buf, axis, me, n, k):
        for j in range(1, n):
            pltpu.make_async_remote_copy(
                src_ref=buf.at[me], dst_ref=buf.at[me], send_sem=ssem.at[k], recv_sem=rsem.at[k],
                device_id={axis: lax.rem(me + j, n)}, device_id_type=MESH,
            ).start()

    def scatter(src, dst, axis, me, n, k):
        for j in range(1, n):
            peer = lax.rem(me + j, n)
            pltpu.make_async_remote_copy(
                src_ref=src.at[peer], dst_ref=dst.at[j - 1], send_sem=ssem.at[k], recv_sem=rsem.at[k],
                device_id={axis: peer}, device_id_type=MESH,
            ).start()

    def share(src, dst, axis, me, n, k):
        for j in range(1, n):
            pltpu.make_async_remote_copy(
                src_ref=src, dst_ref=dst.at[j - 1], send_sem=ssem.at[k], recv_sem=rsem.at[k],
                device_id={axis: lax.rem(me + j, n)}, device_id_type=MESH,
            ).start()

    def wait_for(ref, sem):
        pltpu.make_async_copy(ref, ref, sem).wait()

    def product(x, w, c0):
        for c, width in col_tiles(w.shape[1]):
            part[:, c0 + c : c0 + c + width] = jnp.dot(x, w[:, c : c + width], preferred_element_type=F32)

    def squares(x, c0):
        sq = jnp.broadcast_to(jnp.sum(x * x, axis=1, keepdims=True), (rows, 128))
        high = sq.astype(BF16).astype(F32)
        part[:, c0 : c0 + 128] = high
        part[:, c0 + 128 : c0 + 256] = sq - high

    def stage(dst, width):
        for i in range(n_tp):
            dst[i] = part[i * S : (i + 1) * S, 0:width].astype(BF16)

    def total(sent, got, c, width):
        acc = sent[b, :, c : c + width].astype(F32)
        for j in range(n_tp - 1):
            acc = acc + got[j, :, c : c + width].astype(F32)
        return acc

    def rounded(v):
        return v.astype(BF16).astype(F32)

    loads[0].wait()
    gather(hslots, "kv", a, n_kv, 0)
    wait_for(hslots.at[pl.ds(0, n_kv - 1)], rsem.at[0])
    for i in range(n_kv):
        x16[i * R : (i + 1) * R, :] = hslots[i].astype(F32)
    stream = x16[...]
    scaled_in = (stream * mg[...]).astype(BF16)
    NQ = wq.shape[1]
    NV = wv.shape[1]
    loads[1].wait()
    product(scaled_in, vq, 0)
    loads[2].wait()
    product(scaled_in, vk, NQ)
    squares(stream, 2 * NQ)
    stage(sA, 2 * NQ + 256)
    scatter(sA, rA, "tp", b, n_tp, 1)
    loads[3].wait()
    product(scaled_in, vv, 0)
    loads[4].wait()
    product(scaled_in, vg, NV)
    stage(sB, 2 * NV)
    scatter(sB, rB, "tp", b, n_tp, 2)

    PR = qs.shape[0]
    row = lax.broadcasted_iota(jnp.int32, (PR, 1), 0)
    rate = jnp.zeros((PR, 1), F32)
    filled = jnp.zeros((PR, 1), jnp.int32)
    for h in range(H):
        for s in range(S):
            rate = jnp.where(row == h * S + s, decay[h], rate)
            filled = jnp.where(row == h * S + s, lax.rem(lens[s], BLK), filled)
    slot = lax.broadcasted_iota(jnp.int32, (PR, BLK), 1)
    distance = (filled - slot).astype(F32)
    weighting = jnp.where(slot < filled, jnp.exp(-rate * distance), 0.0)
    carried = jnp.exp(-rate * (filled + 1).astype(F32))
    eye = jnp.where(
        lax.broadcasted_iota(jnp.int32, (DK, DK), 0) == lax.broadcasted_iota(jnp.int32, (DK, DK), 1), 1.0, 0.0
    ).astype(BF16)

    wait_for(rA, rsem.at[1])
    sq = total(sA, rA, 2 * NQ, 128) + total(sA, rA, 2 * NQ + 128, 128)
    scale = lax.rsqrt(sq[:, 0:1] / D + EPS)
    cs = cos[...]
    sn = sin[...]
    for h in range(H):
        for base, dst, factor in ((0, qs, 1.0), (NQ, ks, DK ** (-0.5))):
            front = rounded(scale * total(sA, rA, base + h * DK, half))
            back = rounded(scale * total(sA, rA, base + h * DK + half, half))
            dst[h * S : (h + 1) * S, 0:half] = (front * cs - back * sn) * factor
            dst[h * S : (h + 1) * S, half:DK] = (front * sn + back * cs) * factor
    q8 = qs[...].astype(BF16)
    q8f = q8.astype(F32)
    own = jnp.sum(q8f * ks[...], axis=1, keepdims=True)
    contract_last = (((1,), (1,)), ((), ()))
    loads[6].wait()
    scores = jnp.zeros((PR, BLK), F32)
    for h in range(H):
        for s in range(S):
            one = lax.dot_general(q8, kbv[s, h], contract_last, preferred_element_type=F32)
            scores = jnp.where(row == h * S + s, one, scores)
    block_weights = (scores * weighting).astype(BF16)
    q_columns = lax.dot_general(eye, q8, contract_last, preferred_element_type=F32)
    loads[5].wait()
    for h in range(H):
        for s in range(S):
            i = h * S + s
            column = q_columns[:, i : i + 1]
            for c, width in col_tiles(DV, 128):
                ts[i : i + 1, c : c + width] = jnp.sum(
                    column * st[s, h, :, c : c + width], axis=0, keepdims=True
                )
    loads[7].wait()
    block_term = jnp.zeros((PR, DV), F32)
    for h in range(H):
        for s in range(S):
            one = jnp.dot(block_weights, vbv[s, h], preferred_element_type=F32)
            block_term = jnp.where(row == h * S + s, one, block_term)
    partial = block_term + carried * ts[...]
    wait_for(rB, rsem.at[2])
    for h in range(H):
        vs[h * S : (h + 1) * S, :] = rounded(scale * total(sB, rB, h * DV, DV))
        gs[h * S : (h + 1) * S, :] = rounded(scale * total(sB, rB, NV + h * DV, DV))
    retained = own * vs[...] + partial
    centred = retained - jnp.mean(retained, axis=1, keepdims=True)
    spread = jnp.mean(centred * centred, axis=1, keepdims=True)
    gate = gs[...]
    ts[...] = gate / (1.0 + jnp.exp(-gate)) * (centred * lax.rsqrt(spread + EPS))
    for h in range(H):
        mx[b, :, h * DV : (h + 1) * DV] = (
            ts[h * S : (h + 1) * S, :] * gg[:, h * DV : (h + 1) * DV]
        ).astype(BF16)
    gather(mx, "tp", b, n_tp, 3)
    wait_for(mx.at[pl.ds(0, n_tp - 1)], rsem.at[3])
    for i in range(n_tp):
        mx16[i * S : (i + 1) * S, :] = mx[i].astype(F32)

    loads[8].wait()
    head_terms = jnp.dot(mx16[...].astype(BF16), vo[...], preferred_element_type=F32)
    oS[...] = head_terms.astype(BF16)
    share(oS, oR, "kv", a, n_kv, 4)
    wait_for(oR, rsem.at[4])
    middle = x16[...] + oS[...].astype(F32)
    for j in range(n_kv - 1):
        middle = middle + oR[j].astype(F32)
    x16[...] = middle
    for i in range(n_kv):
        mid[i] = x16[i * R : (i + 1) * R, :]

    scaled_mid = (middle * cg[...]).astype(BF16)
    loads[9].wait()
    product(scaled_mid, vgate, 0)
    loads[10].wait()
    product(scaled_mid, vup, FP)
    squares(middle, 2 * FP)
    stage(sC, 2 * FP + 256)
    scatter(sC, rC, "tp", b, n_tp, 5)
    wait_for(rC, rsem.at[5])
    sq = total(sC, rC, 2 * FP, 128) + total(sC, rC, 2 * FP + 128, 128)
    scale = lax.rsqrt(sq[:, 0:1] / D + EPS)
    for c, width in col_tiles(FL):
        gate = scale * total(sC, rC, c, width)
        up = scale * total(sC, rC, FP + c, width)
        ac[b, :, c : c + width] = (gate / (1.0 + jnp.exp(-gate)) * up).astype(BF16)
    gather(ac, "tp", b, n_tp, 6)
    wait_for(ac.at[pl.ds(0, n_tp - 1)], rsem.at[6])
    for i in range(n_tp):
        ac16[i * S : (i + 1) * S, :] = ac[i].astype(F32)
    loads[11].wait()
    x16[...] = jnp.dot(ac16[...].astype(BF16), vdown[...], preferred_element_type=F32)
    for i in range(n_kv):
        fS[i] = x16[i * R : (i + 1) * R, :].astype(BF16)
    scatter(fS, fR, "kv", a, n_kv, 7)
    wait_for(fR, rsem.at[7])
    result = mid[a] + fS[a].astype(F32)
    for j in range(n_kv - 1):
        result = result + fR[j].astype(F32)
    out[...] = result.astype(BF16)

    for ref, k in (
        (hslots.at[pl.ds(0, n_kv - 1)], 0), (rA, 1), (rB, 2), (mx.at[pl.ds(0, n_tp - 1)], 3), (oR, 4),
        (rC, 5), (ac.at[pl.ds(0, n_tp - 1)], 6), (fR, 7),
    ):
        wait_for(ref, ssem.at[k])


def local(
    n_kv, n_tp,
    hidden_in, mixer_gain, query_weight, key_weight, value_weight, gate_weight, decay_rate, prior_state,
    key_block, value_block, lengths, group_gain, output_weight, channel_gain, hidden_gate, hidden_up, hidden_down,
):
    R, F = hidden_in.shape
    S = lengths.shape[0]
    H = decay_rate.shape[0]
    rows = R * n_kv
    DK, DV = prior_state.shape[2:]
    NQ = query_weight.shape[1]
    NV = value_weight.shape[1]
    FL = hidden_gate.shape[1]
    FP = up128(FL)
    half = DK // 2
    inverse = 10000.0 ** (-jnp.arange(half, dtype=F32) / half)
    angles = lengths.astype(F32)[:, None] * inverse
    pairs = max(8, H * S)
    any_space = pl.BlockSpec(memory_space=pl.ANY)
    vmem = pl.BlockSpec(memory_space=pltpu.VMEM)
    smem = pl.BlockSpec(memory_space=pltpu.SMEM)

    def like(v):
        return pltpu.VMEM(v.shape, v.dtype)

    scratch = [
        pltpu.VMEM((n_kv, R, F), BF16),
        like(query_weight), like(key_weight), like(value_weight), like(gate_weight), like(prior_state),
        like(key_block), like(value_block), like(output_weight), like(hidden_gate), like(hidden_up),
        like(hidden_down),
        pltpu.VMEM((rows, F), F32),
        pltpu.VMEM((rows, max(2 * NQ + 256, 2 * NV, 2 * FP + 256)), F32),
        pltpu.VMEM((n_tp, S, 2 * NQ + 256), BF16),
        pltpu.VMEM((n_tp - 1, S, 2 * NQ + 256), BF16),
        pltpu.VMEM((n_tp, S, 2 * NV), BF16),
        pltpu.VMEM((n_tp - 1, S, 2 * NV), BF16),
        pltpu.VMEM((pairs, DK), F32),
        pltpu.VMEM((pairs, DK), F32),
        pltpu.VMEM((pairs, DV), F32),
        pltpu.VMEM((pairs, DV), F32),
        pltpu.VMEM((pairs, DV), F32),
        pltpu.VMEM((n_tp, S, NV), BF16),
        pltpu.VMEM((rows, NV), F32),
        pltpu.VMEM((rows, F), BF16),
        pltpu.VMEM((n_kv - 1, rows, F), BF16),
        pltpu.VMEM((n_kv, R, F), F32),
        pltpu.VMEM((n_tp, S, 2 * FP + 256), BF16),
        pltpu.VMEM((n_tp - 1, S, 2 * FP + 256), BF16),
        pltpu.VMEM((n_tp, S, FL), BF16),
        pltpu.VMEM((rows, FL), F32),
        pltpu.VMEM((n_kv, R, F), BF16),
        pltpu.VMEM((n_kv - 1, R, F), BF16),
        pltpu.SemaphoreType.DMA((12,)),
        pltpu.SemaphoreType.DMA((8,)),
        pltpu.SemaphoreType.DMA((8,)),
    ]
    return pl.pallas_call(
        functools.partial(layer_kernel, n_kv, n_tp, H),
        out_shape=jax.ShapeDtypeStruct((R, F), BF16),
        in_specs=[
            any_space, vmem, any_space, any_space, any_space, any_space, smem, any_space, any_space, any_space,
            smem, vmem, any_space, vmem, any_space, any_space, any_space, vmem, vmem,
        ],
        out_specs=vmem,
        scratch_shapes=scratch,
        compiler_params=pltpu.CompilerParams(
            collective_id=0, has_side_effects=True, vmem_limit_bytes=60 * 1024 * 1024
        ),
    )(
        hidden_in, mixer_gain[None, :], query_weight, key_weight, value_weight, gate_weight, decay_rate,
        prior_state, key_block, value_block, lengths, group_gain[None, :], output_weight,
        channel_gain[None, :], hidden_gate, hidden_up, hidden_down, jnp.cos(angles), jnp.sin(angles),
    )


def solution(mesh):
    in_specs = (
        P("kv", "tp"), P("tp"), P("tp", "kv"), P("tp", "kv"), P("tp", "kv"), P("tp", "kv"), P("kv"),
        P("tp", "kv", None, None), P("tp", "kv", None, None), P("tp", "kv", None, None), P("tp"), P("kv"),
        P("kv", "tp"), P("tp"), P("tp", "kv"), P("tp", "kv"), P("kv", "tp"),
    )
    body = functools.partial(local, mesh.shape["kv"], mesh.shape["tp"])
    return jax.shard_map(body, mesh=mesh, in_specs=in_specs, out_specs=P("kv", "tp"), check_vma=False)
```

```python
import functools

import jax
import jax.numpy as jnp
import numpy as np
from jax import lax
from jax.experimental import pallas as pl
from jax.experimental.pallas import tpu as pltpu
from jax.sharding import PartitionSpec as P

EPS = 1e-06
CHUNKS = 2
MESH = pl.DeviceIdType.MESH
F32 = jnp.float32
BF16 = jnp.bfloat16


def up128(n):
    return (n + 127) // 128 * 128


def col_tiles(n, width=512):
    return [(c, min(width, n - c)) for c in range(0, n, width)]


def chunks_of(n):
    width = up128(-(-n // CHUNKS))
    return [(c, min(width, n - c)) for c in range(0, n, width)]


def cos_sin(x):
    k = jnp.floor(x * (2.0 / np.pi) + 0.5)
    r = ((x - k * 1.5703125) - k * 4.837512969970703125e-4) - k * 7.54978995489188216e-8
    z = r * r
    sn = ((-1.9515295891e-4 * z + 8.3321608736e-3) * z - 1.6666654611e-1) * z * r + r
    cs = ((2.443315711809948e-5 * z - 1.388731625493765e-3) * z + 4.166664568298827e-2) * z * z - 0.5 * z + 1.0
    turn = k - 4.0 * jnp.floor(k * 0.25)
    odd = (turn == 1.0) | (turn == 3.0)
    cos_sign = jnp.where((turn == 1.0) | (turn == 2.0), -1.0, 1.0)
    sin_sign = jnp.where(turn >= 2.0, -1.0, 1.0)
    return cos_sign * jnp.where(odd, sn, cs), sin_sign * jnp.where(odd, cs, sn)


def layer_kernel(
    n_kv, n_tp, H,
    hid, mg_in, wq, wk, wv, wg, decay_in, state, kblk, vblk, lens_in, gg_in, wo, cg_in, wgate, wup, wdown,
    inverse_in, out,
    mg, gg, cg, inverse, decay, lens, hslots, vq, vk, vv, vg, st, kbv, vbv, vo, vgate, vup, vdown,
    x16, part, sA, rA, sB, rB, sG, rG, qs, ks, vs, gs, ts, mx, mx16, oS, oR, mid, fS, fR,
    lsem, ssem, rsem, *chunk_refs,
):
    a = lax.axis_index("kv")
    b = lax.axis_index("tp")
    R, F = hid.shape
    S = lens_in.shape[0]
    rows = R * n_kv
    DK = state.shape[2]
    DV = state.shape[3]
    BLK = kblk.shape[2]
    FL = wgate.shape[1]
    D = F * n_tp
    half = DK // 2
    pieces = chunks_of(FL)
    sC, rC, ac, ac16 = (chunk_refs[i :: 4] for i in range(4))

    def peers(axis, me, n):
        if axis == "kv":
            return [(lax.rem(me + j, n), j - 1) for j in range(1, n)]
        chips = n // 2
        chip, core = me // 2, lax.rem(me, 2)
        upper = chip // (chips // 2)
        found = []
        for i in range(chips - 1):
            rising = i + (i - chip + chips) // chips
            down = chips - 1 - i
            falling = down - (chip - down + chips) // chips
            other = falling + upper * (rising - falling)
            for same in (0, 1):
                found.append(other * 2 + lax.rem(core + same, 2))
        found.append(chip * 2 + 1 - core)
        return [(peer, lax.rem(peer - me + n, n) - 1) for peer in found]

    barrier = pltpu.get_barrier_semaphore()
    for axis, me, n in (("tp", b, n_tp), ("kv", a, n_kv)):
        for peer, _ in peers(axis, me, n):
            pl.semaphore_signal(barrier, inc=1, device_id={axis: peer}, device_id_type=MESH)

    loads = [
        pltpu.make_async_copy(src, dst, lsem.at[i])
        for i, (src, dst) in enumerate(
            [
                (hid, hslots.at[a]), (wq, vq), (wk, vk), (wv, vv), (wg, vg), (state, st),
                (kblk, kbv), (vblk, vbv), (wo, vo), (wgate, vgate), (wup, vup), (wdown, vdown),
                (mg_in, mg), (lens_in, lens), (decay_in, decay), (inverse_in, inverse), (gg_in, gg), (cg_in, cg),
            ]
        )
    ]
    for i in (0, 12, 1, 2, 3, 4, 13, 14, 15, 6, 5, 7, 16, 8, 17, 9, 10, 11):
        loads[i].start()
    pl.semaphore_wait(barrier, n_kv + n_tp - 2)

    def gather(buf, axis, me, n, k):
        for peer, _ in peers(axis, me, n):
            pltpu.make_async_remote_copy(
                src_ref=buf.at[me], dst_ref=buf.at[me], send_sem=ssem.at[k], recv_sem=rsem.at[k],
                device_id={axis: peer}, device_id_type=MESH,
            ).start()

    def scatter(src, dst, axis, me, n, k):
        for peer, slot in peers(axis, me, n):
            pltpu.make_async_remote_copy(
                src_ref=src.at[peer], dst_ref=dst.at[slot], send_sem=ssem.at[k], recv_sem=rsem.at[k],
                device_id={axis: peer}, device_id_type=MESH,
            ).start()

    def share(src, dst, axis, me, n, k):
        for j in range(1, n):
            pltpu.make_async_remote_copy(
                src_ref=src, dst_ref=dst.at[j - 1], send_sem=ssem.at[k], recv_sem=rsem.at[k],
                device_id={axis: lax.rem(me + j, n)}, device_id_type=MESH,
            ).start()

    def wait_for(ref, sem):
        pltpu.make_async_copy(ref, ref, sem).wait()

    def product(x, w, c0, first=0, extent=None):
        for c, width in col_tiles(w.shape[1] if extent is None else extent):
            part[:, c0 + c : c0 + c + width] = jnp.dot(
                x, w[:, first + c : first + c + width], preferred_element_type=F32
            )

    def squares(x, c0):
        sq = jnp.broadcast_to(jnp.sum(x * x, axis=1, keepdims=True), (rows, 128))
        high = sq.astype(BF16).astype(F32)
        part[:, c0 : c0 + 128] = high
        part[:, c0 + 128 : c0 + 256] = sq - high

    def stage(dst, width):
        for i in range(n_tp):
            dst[i] = part[i * S : (i + 1) * S, 0:width].astype(BF16)

    def total(sent, got, c, width):
        acc = sent[b, :, c : c + width].astype(F32)
        for j in range(n_tp - 1):
            acc = acc + got[j, :, c : c + width].astype(F32)
        return acc

    def rounded(v):
        return v.astype(BF16).astype(F32)

    loads[0].wait()
    gather(hslots, "kv", a, n_kv, 0)
    wait_for(hslots.at[pl.ds(0, n_kv - 1)], rsem.at[0])
    for i in range(n_kv):
        x16[i * R : (i + 1) * R, :] = hslots[i].astype(F32)
    stream = x16[...]
    loads[12].wait()
    scaled_in = (stream * mg[...]).astype(BF16)
    NQ = wq.shape[1]
    NV = wv.shape[1]
    loads[1].wait()
    product(scaled_in, vq, 0)
    loads[2].wait()
    product(scaled_in, vk, NQ)
    squares(stream, 2 * NQ)
    stage(sA, 2 * NQ + 256)
    scatter(sA, rA, "tp", b, n_tp, 1)
    loads[3].wait()
    product(scaled_in, vv, 0)
    stage(sB, NV)
    scatter(sB, rB, "tp", b, n_tp, 2)
    loads[4].wait()
    product(scaled_in, vg, 0)
    stage(sG, NV)
    scatter(sG, rG, "tp", b, n_tp, 5)

    PR = qs.shape[0]
    for i in (13, 14, 15):
        loads[i].wait()
    row = lax.broadcasted_iota(jnp.int32, (PR, 1), 0)
    rate = jnp.zeros((PR, 1), F32)
    filled = jnp.zeros((PR, 1), jnp.int32)
    for h in range(H):
        for s in range(S):
            rate = jnp.where(row == h * S + s, decay[h], rate)
            filled = jnp.where(row == h * S + s, lax.rem(lens[s], BLK), filled)
    slot = lax.broadcasted_iota(jnp.int32, (PR, BLK), 1)
    distance = (filled - slot).astype(F32)
    weighting = jnp.where(slot < filled, jnp.exp(-rate * distance), 0.0)
    carried = jnp.exp(-rate * (filled + 1).astype(F32))
    seq = lax.broadcasted_iota(jnp.int32, (S, half), 0)
    position = jnp.zeros((S, half), F32)
    for s in range(S):
        position = jnp.where(seq == s, lens[s].astype(F32), position)
    cs, sn = cos_sin(position * inverse[...])
    eye = jnp.where(
        lax.broadcasted_iota(jnp.int32, (DK, DK), 0) == lax.broadcasted_iota(jnp.int32, (DK, DK), 1), 1.0, 0.0
    ).astype(BF16)

    wait_for(rA, rsem.at[1])
    sq = total(sA, rA, 2 * NQ, 128) + total(sA, rA, 2 * NQ + 128, 128)
    scale = lax.rsqrt(sq[:, 0:1] / D + EPS)
    for h in range(H):
        for base, dst, factor in ((0, qs, 1.0), (NQ, ks, DK ** (-0.5))):
            front = rounded(scale * total(sA, rA, base + h * DK, half))
            back = rounded(scale * total(sA, rA, base + h * DK + half, half))
            dst[h * S : (h + 1) * S, 0:half] = (front * cs - back * sn) * factor
            dst[h * S : (h + 1) * S, half:DK] = (front * sn + back * cs) * factor
    q8 = qs[...].astype(BF16)
    q8f = q8.astype(F32)
    own = jnp.sum(q8f * ks[...], axis=1, keepdims=True)
    contract_last = (((1,), (1,)), ((), ()))
    loads[6].wait()
    scores = jnp.zeros((PR, BLK), F32)
    for h in range(H):
        for s in range(S):
            one = lax.dot_general(q8, kbv[s, h], contract_last, preferred_element_type=F32)
            scores = jnp.where(row == h * S + s, one, scores)
    block_weights = (scores * weighting).astype(BF16)
    q_columns = lax.dot_general(eye, q8, contract_last, preferred_element_type=F32)
    loads[5].wait()
    for h in range(H):
        for s in range(S):
            i = h * S + s
            column = q_columns[:, i : i + 1]
            for c, width in col_tiles(DV, 128):
                ts[i : i + 1, c : c + width] = jnp.sum(
                    column * st[s, h, :, c : c + width], axis=0, keepdims=True
                )
    loads[7].wait()
    block_term = jnp.zeros((PR, DV), F32)
    for h in range(H):
        for s in range(S):
            one = jnp.dot(block_weights, vbv[s, h], preferred_element_type=F32)
            block_term = jnp.where(row == h * S + s, one, block_term)
    partial = block_term + carried * ts[...]
    wait_for(rB, rsem.at[2])
    for h in range(H):
        vs[h * S : (h + 1) * S, :] = rounded(scale * total(sB, rB, h * DV, DV))
    retained = own * vs[...] + partial
    centred = retained - jnp.mean(retained, axis=1, keepdims=True)
    spread = jnp.mean(centred * centred, axis=1, keepdims=True)
    loads[16].wait()
    wait_for(rG, rsem.at[5])
    for h in range(H):
        gs[h * S : (h + 1) * S, :] = rounded(scale * total(sG, rG, h * DV, DV))
    gate = gs[...]
    ts[...] = gate / (1.0 + jnp.exp(-gate)) * (centred * lax.rsqrt(spread + EPS))
    for h in range(H):
        mx[b, :, h * DV : (h + 1) * DV] = (
            ts[h * S : (h + 1) * S, :] * gg[:, h * DV : (h + 1) * DV]
        ).astype(BF16)
    gather(mx, "tp", b, n_tp, 3)
    wait_for(mx.at[pl.ds(0, n_tp - 1)], rsem.at[3])
    for i in range(n_tp):
        mx16[i * S : (i + 1) * S, :] = mx[i].astype(F32)

    loads[8].wait()
    head_terms = jnp.dot(mx16[...].astype(BF16), vo[...], preferred_element_type=F32)
    oS[...] = head_terms.astype(BF16)
    share(oS, oR, "kv", a, n_kv, 4)
    wait_for(oR, rsem.at[4])
    middle = x16[...] + oS[...].astype(F32)
    for j in range(n_kv - 1):
        middle = middle + oR[j].astype(F32)
    x16[...] = middle
    for i in range(n_kv):
        mid[i] = x16[i * R : (i + 1) * R, :]

    loads[17].wait()
    scaled_mid = (middle * cg[...]).astype(BF16)
    loads[9].wait()
    loads[10].wait()
    for n, (first, extent) in enumerate(pieces):
        wide = up128(extent)
        product(scaled_mid, vgate, 0, first, extent)
        product(scaled_mid, vup, wide, first, extent)
        if n == 0:
            squares(middle, 2 * wide)
        stage(sC[n], sC[n].shape[2])
        scatter(sC[n], rC[n], "tp", b, n_tp, 8 + 2 * n)
    for n, (first, extent) in enumerate(pieces):
        wide = up128(extent)
        wait_for(rC[n], rsem.at[8 + 2 * n])
        if n == 0:
            sq = total(sC[0], rC[0], 2 * wide, 128) + total(sC[0], rC[0], 2 * wide + 128, 128)
            scale = lax.rsqrt(sq[:, 0:1] / D + EPS)
        for c, width in col_tiles(extent):
            gate = scale * total(sC[n], rC[n], c, width)
            up = scale * total(sC[n], rC[n], wide + c, width)
            ac[n][b, :, c : c + width] = (gate / (1.0 + jnp.exp(-gate)) * up).astype(BF16)
        gather(ac[n], "tp", b, n_tp, 9 + 2 * n)
    loads[11].wait()
    for n, (first, extent) in enumerate(pieces):
        wait_for(ac[n].at[pl.ds(0, n_tp - 1)], rsem.at[9 + 2 * n])
        for i in range(n_tp):
            ac16[n][i * S : (i + 1) * S, :] = ac[n][i].astype(F32)
        unit_terms = jnp.dot(
            ac16[n][...].astype(BF16), vdown[first : first + extent, :], preferred_element_type=F32
        )
        x16[...] = unit_terms if n == 0 else x16[...] + unit_terms
    for i in range(n_kv):
        fS[i] = x16[i * R : (i + 1) * R, :].astype(BF16)
    scatter(fS, fR, "kv", a, n_kv, 7)
    wait_for(fR, rsem.at[7])
    result = mid[a] + fS[a].astype(F32)
    for j in range(n_kv - 1):
        result = result + fR[j].astype(F32)
    out[...] = result

    sent = [
        (hslots.at[pl.ds(0, n_kv - 1)], 0), (rA, 1), (rB, 2), (mx.at[pl.ds(0, n_tp - 1)], 3), (oR, 4),
        (rG, 5), (fR, 7),
    ]
    for n in range(len(pieces)):
        sent += [(rC[n], 8 + 2 * n), (ac[n].at[pl.ds(0, n_tp - 1)], 9 + 2 * n)]
    for ref, k in sent:
        wait_for(ref, ssem.at[k])


def local(
    n_kv, n_tp,
    hidden_in, mixer_gain, query_weight, key_weight, value_weight, gate_weight, decay_rate, prior_state,
    key_block, value_block, lengths, group_gain, output_weight, channel_gain, hidden_gate, hidden_up, hidden_down,
):
    R, F = hidden_in.shape
    S = lengths.shape[0]
    H = decay_rate.shape[0]
    rows = R * n_kv
    DK, DV = prior_state.shape[2:]
    NQ = query_weight.shape[1]
    NV = value_weight.shape[1]
    FL = hidden_gate.shape[1]
    half = DK // 2
    pieces = chunks_of(FL)
    inverse = jnp.asarray((10000.0 ** (-np.arange(half) / half)).astype(np.float32)[None, :])
    pairs = max(8, H * S)
    any_space = pl.BlockSpec(memory_space=pl.ANY)
    vmem = pl.BlockSpec(memory_space=pltpu.VMEM)

    def like(v):
        return pltpu.VMEM(v.shape, v.dtype)

    scratch = [
        pltpu.VMEM((1, F), F32),
        pltpu.VMEM((1, NV), F32),
        pltpu.VMEM((1, F), F32),
        pltpu.VMEM((1, half), F32),
        pltpu.SMEM((H,), F32),
        pltpu.SMEM((S,), jnp.int32),
        pltpu.VMEM((n_kv, R, F), BF16),
        like(query_weight), like(key_weight), like(value_weight), like(gate_weight), like(prior_state),
        like(key_block), like(value_block), like(output_weight), like(hidden_gate), like(hidden_up),
        like(hidden_down),
        pltpu.VMEM((rows, F), F32),
        pltpu.VMEM((rows, max(2 * NQ + 256, 2 * NV, 2 * up128(pieces[0][1]) + 256)), F32),
        pltpu.VMEM((n_tp, S, 2 * NQ + 256), BF16),
        pltpu.VMEM((n_tp - 1, S, 2 * NQ + 256), BF16),
        pltpu.VMEM((n_tp, S, NV), BF16),
        pltpu.VMEM((n_tp - 1, S, NV), BF16),
        pltpu.VMEM((n_tp, S, NV), BF16),
        pltpu.VMEM((n_tp - 1, S, NV), BF16),
        pltpu.VMEM((pairs, DK), F32),
        pltpu.VMEM((pairs, DK), F32),
        pltpu.VMEM((pairs, DV), F32),
        pltpu.VMEM((pairs, DV), F32),
        pltpu.VMEM((pairs, DV), F32),
        pltpu.VMEM((n_tp, S, NV), BF16),
        pltpu.VMEM((rows, NV), F32),
        pltpu.VMEM((rows, F), BF16),
        pltpu.VMEM((n_kv - 1, rows, F), BF16),
        pltpu.VMEM((n_kv, R, F), F32),
        pltpu.VMEM((n_kv, R, F), BF16),
        pltpu.VMEM((n_kv - 1, R, F), BF16),
        pltpu.SemaphoreType.DMA((18,)),
        pltpu.SemaphoreType.DMA((8 + 2 * len(pieces),)),
        pltpu.SemaphoreType.DMA((8 + 2 * len(pieces),)),
    ]
    for n, (_, extent) in enumerate(pieces):
        columns = 2 * up128(extent) + (256 if n == 0 else 0)
        scratch += [
            pltpu.VMEM((n_tp, S, columns), BF16),
            pltpu.VMEM((n_tp - 1, S, columns), BF16),
            pltpu.VMEM((n_tp, S, extent), BF16),
            pltpu.VMEM((rows, extent), F32),
        ]
    return pl.pallas_call(
        functools.partial(layer_kernel, n_kv, n_tp, H),
        out_shape=jax.ShapeDtypeStruct((R, F), F32),
        in_specs=[any_space] * 18,
        out_specs=vmem,
        scratch_shapes=scratch,
        compiler_params=pltpu.CompilerParams(
            collective_id=0, has_side_effects=True, vmem_limit_bytes=60 * 1024 * 1024
        ),
    )(
        hidden_in, mixer_gain[None, :], query_weight, key_weight, value_weight, gate_weight, decay_rate,
        prior_state, key_block, value_block, lengths, group_gain[None, :], output_weight,
        channel_gain[None, :], hidden_gate, hidden_up, hidden_down, inverse,
    ).astype(BF16)


def solution(mesh):
    in_specs = (
        P("kv", "tp"), P("tp"), P("tp", "kv"), P("tp", "kv"), P("tp", "kv"), P("tp", "kv"), P("kv"),
        P("tp", "kv", None, None), P("tp", "kv", None, None), P("tp", "kv", None, None), P("tp"), P("kv"),
        P("kv", "tp"), P("tp"), P("tp", "kv"), P("tp", "kv"), P("kv", "tp"),
    )
    body = functools.partial(local, mesh.shape["kv"], mesh.shape["tp"])
    return jax.shard_map(body, mesh=mesh, in_specs=in_specs, out_specs=P("kv", "tp"), check_vma=False)
```
